32 devices in a mesh: sp: 16 (over z, y, x), tp: 2 (over core).
Axes of the slice: x: 2, y: 2, z: 4, core: 2. Of those that a mesh axis runs over, the one named last changes fastest.
Arguments:
- resid: bfloat16 [4096, 2048], P('sp', 'tp'), may hold values from -6 to 6
- queries: bfloat16 [4096, 1024], P('sp', 'tp'), may hold values from -6 to 6
- keys_values: bfloat16 [8, 4096, 128], P('tp', 'sp'), may hold values from -6 to 6
- cum_gate: float32 [16, 4096], P('tp', 'sp'), as said below
- out_weight: bfloat16 [1024, 2048], P(None, 'tp'), may hold values from -1.5 to 1.5
- norm_gain: float32 [2048], replicated, may hold values from 0.1 to 1.9
- gate_weight: bfloat16 [2048, 5632], P('sp', 'tp'), may hold values from -0.125 to 0.125
- up_weight: bfloat16 [2048, 5632], P('sp', 'tp'), may hold values from -0.125 to 0.125
- conv_kernel: float32 [3, 2, 5632], P(None, None, 'tp'), may hold values from -3.5 to 3.5
- down_weight: bfloat16 [5632, 2048], P('tp', 'sp'), may hold values from -0.078125 to 0.078125
Outputs:
- layer_out: bfloat16 [4096, 2048], P('sp', 'tp')
The draws below stay inside these ranges and needn't reach their ends.
Inputs may be any that keep to these rules, and one draw needn't show every extreme that they name: `cum_gate`: along positions each head's entries never increase.
All inputs are finite; a program needn't handle non-finite values.
Results may differ from the reference program's by a relative error of at most 0.015.
Values may be sent and summed in bfloat16 or wider, within the bound.
A program may use at most 128 MiB of HBM per device.

```python
import math
import jax
import jax.numpy as jnp
from jax import lax

D = 2048
QUERY_HEAD_COUNT = 16
KV_HEADS = 8
HD = 64
FF = 5632
KSIZE = 3
TOK_DEV = 256
SEQUENCE_TOKENS = 4096


def draw_queries(key, part):
    drawn = jnp.clip(jax.random.normal(jax.random.fold_in(key, 1), (SEQUENCE_TOKENS, QUERY_HEAD_COUNT * HD), jnp.float32), -5.9, 5.9)
    return drawn.astype(jnp.bfloat16)


def draw_keys_values(key, part):
    drawn = jnp.clip(jax.random.normal(jax.random.fold_in(key, 2), (KV_HEADS, SEQUENCE_TOKENS, 2 * HD), jnp.float32), -5.9, 5.9)
    return drawn.astype(jnp.bfloat16)


def draw_cum_gate(key, part):
    order = jax.random.permutation(jax.random.fold_in(key, 11), QUERY_HEAD_COUNT)
    quick_decay_heads = order < QUERY_HEAD_COUNT // 2
    fast_rate = jnp.exp(jax.random.uniform(jax.random.fold_in(key, 12), (QUERY_HEAD_COUNT,), jnp.float32, jnp.log(1.0 / 100.0), jnp.log(1.0 / 30.0)))
    slow_total = jnp.exp(jax.random.uniform(jax.random.fold_in(key, 13), (QUERY_HEAD_COUNT,), jnp.float32, jnp.log(0.3), jnp.log(0.8)))
    baseline_decay = jnp.where(quick_decay_heads, fast_rate, slow_total / SEQUENCE_TOKENS)
    jitter_amplitude = jnp.exp(jax.random.uniform(jax.random.fold_in(key, 14), (QUERY_HEAD_COUNT, SEQUENCE_TOKENS), jnp.float32, jnp.log(0.5), jnp.log(2.0)))
    block_multiplier = jnp.exp(jax.random.uniform(jax.random.fold_in(key, 15), (QUERY_HEAD_COUNT, SEQUENCE_TOKENS // TOK_DEV), jnp.float32, jnp.log(0.5), jnp.log(2.0)))
    block_multiplier = jnp.repeat(block_multiplier, TOK_DEV, axis=1)
    spike_locations = jax.random.randint(jax.random.fold_in(key, 16), (2,), 1, SEQUENCE_TOKENS)
    token_places = jnp.arange(SEQUENCE_TOKENS)
    spike_active = (token_places[:, None] == spike_locations[None, :]).any(axis=1)
    spike_penalty = jax.random.uniform(jax.random.fold_in(key, 17), (QUERY_HEAD_COUNT, SEQUENCE_TOKENS), jnp.float32, 0.2, 0.4)
    spike_addend = jnp.where(spike_active[None, :] & jnp.logical_not(quick_decay_heads)[:, None], jnp.log(1.0 - spike_penalty), 0.0)
    gate_logarithm = -baseline_decay[:, None] * jitter_amplitude * block_multiplier + spike_addend
    return jnp.cumsum(gate_logarithm, axis=1).astype(jnp.float32)


def steps_of(own_key, shape, pieces, low, high):
    gain, own = 1.0, jax.random.fold_in(own_key, 6)
    for axis_at, parts in pieces:
        steps = jnp.exp(jax.random.uniform(jax.random.fold_in(own, axis_at), (parts,), jnp.float32, low / len(pieces), high / len(pieces)))
        gain = gain * jnp.repeat(steps, shape[axis_at] // parts).reshape([-1 if axis == axis_at else 1 for axis in range(len(shape))])
    return gain


def gaussian(stream_key, extent, width, limit, pieces=(), held_as=jnp.bfloat16):
    loudness = steps_of(stream_key, extent, pieces, -0.22, 0.18) if pieces else 1.0
    array = jax.random.normal(stream_key, extent, jnp.float32) * width * loudness
    return jnp.minimum(jnp.maximum(array, -limit), limit).astype(held_as)


def setup_inputs(seed: int = 0) -> dict:
    splits = jax.random.split(jax.random.key(seed), 11)
    resid = gaussian(splits[0], (SEQUENCE_TOKENS, D), 1.0, 6.0, ((0, 16), (1, 2)))
    queries = draw_queries(jax.random.fold_in(splits[10], 71), 0)
    keys_values = draw_keys_values(jax.random.fold_in(splits[10], 71), 0)
    cum_gate = draw_cum_gate(jax.random.fold_in(splits[10], 71), 0)
    out_weight = gaussian(splits[4], (QUERY_HEAD_COUNT * HD, D), 0.25, 1.5, ((1, 2),))
    norm_gain = jnp.clip(1.0 + 0.18 * jax.random.normal(splits[5], (D,), jnp.float32), 0.1, 1.9)
    gate_weight = gaussian(splits[6], (D, FF), D ** -0.5, 0.125, ((0, 16), (1, 2)))
    up_weight = gaussian(splits[7], (D, FF), D ** -0.5, 0.125, ((0, 16), (1, 2)))
    conv_kernel = gaussian(splits[8], (KSIZE, 2, FF), KSIZE ** -0.5, 3.5, ((2, 2),), jnp.float32)
    down_weight = gaussian(splits[9], (FF, D), FF ** -0.5, 0.078125, ((0, 2), (1, 16)))
    return dict(resid=resid, queries=queries, keys_values=keys_values, cum_gate=cum_gate, out_weight=out_weight, norm_gain=norm_gain, gate_weight=gate_weight, up_weight=up_weight, conv_kernel=conv_kernel, down_weight=down_weight)


norm_eps = 1e-06

def reference(resid, queries, keys_values, cum_gate, out_weight, norm_gain, gate_weight, up_weight, conv_kernel, down_weight):
    group_size = QUERY_HEAD_COUNT // KV_HEADS
    score_scale = HD ** (-0.5)
    query_rows = math.gcd(SEQUENCE_TOKENS, 512)
    block_count = SEQUENCE_TOKENS // query_rows
    key_positions = jnp.arange(SEQUENCE_TOKENS, dtype=jnp.int32)

    def one_item(item_index):
        head = item_index // block_count
        block = item_index % block_count
        first = (block * query_rows).astype(jnp.int32)
        query_part = lax.dynamic_slice(queries, (first, (head * HD).astype(jnp.int32)), (query_rows, HD))
        pair = lax.dynamic_index_in_dim(keys_values, (head // group_size).astype(jnp.int32), 0, keepdims=False)
        key_rows = pair[:, :HD]
        value_rows = pair[:, HD:]
        head_gates = lax.dynamic_index_in_dim(cum_gate, head.astype(jnp.int32), 0, keepdims=False)
        query_gates = lax.dynamic_slice_in_dim(head_gates, first, query_rows)
        scores = jnp.dot(query_part, key_rows.T, preferred_element_type=jnp.float32) * score_scale
        scores = scores + query_gates[:, None] - head_gates[None, :]
        query_positions = first + jnp.arange(query_rows, dtype=jnp.int32)
        visible = key_positions[None, :] <= query_positions[:, None]
        row_max = lax.optimization_barrier(jnp.max(jnp.where(visible, scores, -jnp.inf), axis=1))
        weights = jnp.where(visible, jnp.exp(scores - row_max[:, None]), 0.0)
        row_sum = lax.optimization_barrier(jnp.sum(weights, axis=1))
        result = jnp.dot(weights.astype(jnp.bfloat16), value_rows, preferred_element_type=jnp.float32)
        return result / row_sum[:, None]
    heads_out = lax.map(one_item, jnp.arange(QUERY_HEAD_COUNT * block_count, dtype=jnp.int32))
    heads_out = heads_out.reshape(QUERY_HEAD_COUNT, block_count, query_rows, HD).transpose(1, 2, 0, 3)
    attn = heads_out.reshape(SEQUENCE_TOKENS, QUERY_HEAD_COUNT * HD).astype(jnp.bfloat16)
    middle = (resid.astype(jnp.float32) + jnp.dot(attn, out_weight, preferred_element_type=jnp.float32)).astype(jnp.bfloat16)
    middle_f32 = middle.astype(jnp.float32)
    inverse = lax.rsqrt(lax.optimization_barrier(jnp.mean(middle_f32 * middle_f32, axis=1, keepdims=True)) + norm_eps)
    normed = (middle_f32 * inverse * norm_gain).astype(jnp.bfloat16)
    pre_gate = jnp.dot(normed, gate_weight, preferred_element_type=jnp.float32).astype(jnp.bfloat16)
    pre_up = jnp.dot(normed, up_weight, preferred_element_type=jnp.float32).astype(jnp.bfloat16)
    joined = jnp.concatenate([pre_gate, pre_up], axis=1).astype(jnp.float32)
    padded = jnp.concatenate([jnp.zeros((KSIZE - 1, 2 * FF), jnp.float32), joined], axis=0)
    kernel = conv_kernel.reshape(KSIZE, 2 * FF)
    mixed = jnp.zeros((SEQUENCE_TOKENS, 2 * FF), jnp.float32)
    for offset in range(KSIZE):
        mixed = mixed + kernel[offset][None, :] * padded[offset:offset + SEQUENCE_TOKENS]
    hidden = (jax.nn.silu(mixed[:, :FF]) * mixed[:, FF:]).astype(jnp.bfloat16)
    channel_out = jnp.dot(hidden, down_weight, preferred_element_type=jnp.float32)
    return (middle_f32 + channel_out).astype(jnp.bfloat16)
```

```python
import functools

import jax
import jax.numpy as jnp
from jax import lax
from jax.experimental import pallas as pl
from jax.experimental.pallas import tpu as pltpu
from jax.sharding import PartitionSpec as P

norm_eps = 1e-06
log2e = 1.4426950408889634
MESH = pl.DeviceIdType.MESH
VMEM = pl.BlockSpec(memory_space=pltpu.VMEM)
ANY = pl.BlockSpec(memory_space=pl.ANY)


def send_to(src, dst, send_sem, recv_sem, where):
    return pltpu.make_async_remote_copy(
        src_ref=src,
        dst_ref=dst,
        send_sem=send_sem,
        recv_sem=recv_sem,
        device_id=where,
        device_id_type=MESH,
    )


def attend_kernel(
    n, group, wide, q_ref, kv_ref, gate_ref, wgu_ref, wd_ref,
    out_ref, wgu_out, wd_out,
    kv_all, gate_all, max_s, acc_s,
    kv_send, kv_recv, gate_send, gate_recv, gu_send, gu_recv, dn_send, dn_recv, own_sem,
):
    me = lax.axis_index("sp")
    pairs, rows, width = kv_ref.shape
    per_pair = gate_ref.shape[0] // pairs
    dcols = wd_ref.shape[2]

    barrier = pltpu.get_barrier_semaphore()

    def greet(d, c):
        pl.semaphore_signal(barrier, inc=1, device_id={"sp": lax.rem(me + d, n)}, device_id_type=MESH)
        return c

    lax.fori_loop(1, n, greet, 0)
    pl.semaphore_wait(barrier, n - 1)

    def kv_copy(peer, owner):
        return send_to(kv_ref, kv_all.at[owner], kv_send.at[peer], kv_recv.at[owner], {"sp": peer})

    def gate_copy(peer, owner):
        return send_to(gate_ref, gate_all.at[owner], gate_send.at[peer], gate_recv.at[owner], {"sp": peer})

    def wd_slot(owner):
        if wide:
            return wd_out.at[:, pl.ds(pl.multiple_of(owner * dcols, dcols), dcols)]
        return wd_out.at[owner]

    def gu_copy(peer, owner):
        return send_to(
            wgu_ref.at[lax.rem(peer, group)], wgu_out.at[owner], gu_send.at[peer], gu_recv.at[owner], {"sp": peer}
        )

    def dn_copy(peer, owner):
        return send_to(
            wd_ref.at[lax.rem(peer, group)], wd_slot(owner), dn_send.at[peer], dn_recv.at[owner], {"sp": peer}
        )

    def start_kv(d, c):
        gate_copy(me + d, me).start()
        kv_copy(me + d, me).start()
        return c

    lax.fori_loop(1, n - me, start_kv, 0)

    def start_weights(d, c):
        peer = lax.rem(me + d, n)
        gu_copy(peer, me).start()
        dn_copy(peer, me).start()
        return c

    lax.fori_loop(1, n, start_weights, 0)
    own_gu = pltpu.make_async_copy(wgu_ref.at[lax.rem(me, group)], wgu_out.at[me], own_sem.at[0])
    own_dn = pltpu.make_async_copy(wd_ref.at[lax.rem(me, group)], wd_slot(me), own_sem.at[1])
    own_gu.start()
    own_dn.start()

    lanes = lax.broadcasted_iota(jnp.int32, (rows, width), 1)

    def fold(pair, block, gates, first):
        ones_values = jnp.where(lanes < width // 2, jnp.bfloat16(1.0), block)
        for inner in range(per_pair):
            h = pair * per_pair + inner
            scores = lax.dot_general(
                q_ref[h], block, (((1,), (1,)), ((), ())), preferred_element_type=jnp.float32
            )
            scores = scores * log2e - gates[h : h + 1, :] * log2e
            if first:
                r = lax.broadcasted_iota(jnp.int32, scores.shape, 0)
                c = lax.broadcasted_iota(jnp.int32, scores.shape, 1)
                scores = jnp.where(r >= c, scores, -1e30)
            top = jnp.max(scores, axis=1, keepdims=True)
            if first:
                weights = jnp.exp2(scores - top).astype(jnp.bfloat16)
                acc_s[h] = jnp.dot(weights, ones_values, preferred_element_type=jnp.float32)
                max_s[h] = jnp.broadcast_to(top, (scores.shape[0], width))
            else:
                old = max_s[h]
                top = jnp.maximum(old, top)
                weights = jnp.exp2(scores - top[:, :1]).astype(jnp.bfloat16)
                acc_s[h] = acc_s[h] * jnp.exp2(old - top) + jnp.dot(
                    weights, ones_values, preferred_element_type=jnp.float32
                )
                max_s[h] = top

    own_gates = gate_ref[...]
    for pair in range(pairs):
        fold(pair, kv_ref[pair], own_gates, True)

    def earlier(d, c):
        owner = me - d
        gate_copy(me, owner).wait_recv()
        kv_copy(me, owner).wait_recv()
        gates = gate_all[owner]
        for pair in range(pairs):
            fold(pair, kv_all[owner, pair], gates, False)
        return c

    lax.fori_loop(1, me + 1, earlier, 0)
    for h in range(pairs * per_pair):
        acc = acc_s[h]
        out_ref[h] = (acc[:, width // 2 :] / acc[:, : width // 2]).astype(jnp.bfloat16)

    def end_kv(d, c):
        gate_copy(me + d, me).wait_send()
        kv_copy(me + d, me).wait_send()
        return c

    lax.fori_loop(1, n - me, end_kv, 0)

    def end_weights(d, c):
        peer = lax.rem(me + d, n)
        gu_copy(peer, me).wait_send()
        dn_copy(peer, me).wait_send()
        owner = lax.rem(me - d + n, n)
        gu_copy(owner, owner).wait_recv()
        dn_copy(owner, owner).wait_recv()
        return c

    lax.fori_loop(1, n, end_weights, 0)
    own_gu.wait()
    own_dn.wait()


def attend(queries, keys_values, cum_gate, wgu, wd, n, group):
    tok_rows = queries.shape[0]
    pairs, rows, width = keys_values.shape
    heads = cum_gate.shape[0]
    head_dim = width // 2
    q = (queries * (head_dim**-0.5)).astype(jnp.bfloat16).reshape(tok_rows, heads, head_dim)
    q = jnp.pad(q.transpose(1, 0, 2), ((0, 0), (0, 0), (0, head_dim)))
    _, hid, dcols = wd.shape
    wide = dcols % 128 == 0
    dma = pltpu.SemaphoreType.DMA
    out, wgu_all, wd_all = pl.pallas_call(
        functools.partial(attend_kernel, n, group, wide),
        out_shape=(
            jax.ShapeDtypeStruct((heads, tok_rows, head_dim), jnp.bfloat16),
            jax.ShapeDtypeStruct((n,) + wgu.shape[1:], jnp.bfloat16),
            jax.ShapeDtypeStruct((hid, n * dcols) if wide else (n, hid, dcols), jnp.bfloat16),
        ),
        in_specs=[VMEM] * 5,
        out_specs=(VMEM, ANY, ANY),
        scratch_shapes=[
            pltpu.VMEM((n, pairs, rows, width), jnp.bfloat16),
            pltpu.VMEM((n, heads, rows), jnp.float32),
            pltpu.VMEM((heads, tok_rows, width), jnp.float32),
            pltpu.VMEM((heads, tok_rows, width), jnp.float32),
        ]
        + [dma((n,))] * 8
        + [dma((2,))],
        compiler_params=pltpu.CompilerParams(collective_id=0, has_side_effects=True, vmem_limit_bytes=40 << 20),
        cost_estimate=pl.CostEstimate(flops=10**10, bytes_accessed=10**7, transcendentals=10**7),
        name="attend",
    )(q, keys_values, cum_gate, wgu, wd)
    if not wide:
        wd_all = wd_all.transpose(1, 0, 2).reshape(hid, n * dcols)
    attn = out.transpose(1, 0, 2).reshape(tok_rows, heads * head_dim)
    return attn, wgu_all.reshape(-1, wgu.shape[2]), wd_all


def greet_all(group, tp):
    me, mt = lax.axis_index("sp"), lax.axis_index("tp")
    base = me - lax.rem(me, group)
    barrier = pltpu.get_barrier_semaphore()
    for d in range(1, group):
        peer = base + lax.rem(me + d, group)
        pl.semaphore_signal(barrier, inc=1, device_id={"sp": peer, "tp": mt}, device_id_type=MESH)
    for e in range(1, tp):
        other = lax.rem(mt + e, tp)
        pl.semaphore_signal(barrier, inc=1, device_id={"sp": me, "tp": other}, device_id_type=MESH)
    pl.semaphore_wait(barrier, group + tp - 2)
    return me, mt, base


def gather_kernel(group, tp, x_ref, out_ref, own_sem, s1, r1, s2, r2):
    rows, cols = x_ref.shape
    me, mt, base = greet_all(group, tp)
    mine = lax.rem(me, group)

    def slot(b, t):
        return out_ref.at[
            pl.ds(pl.multiple_of(b * rows, rows), rows), pl.ds(pl.multiple_of(t * cols, cols), cols)
        ]

    def across(peer_b, owner_b):
        return send_to(
            x_ref, slot(owner_b, mt), s1.at[peer_b], r1.at[owner_b], {"sp": base + peer_b, "tp": mt}
        )

    def within(src, b, other, owner_t):
        return send_to(src, slot(b, owner_t), s2.at[b, other], r2.at[b, owner_t], {"sp": me, "tp": other})

    own = pltpu.make_async_copy(x_ref, slot(mine, mt), own_sem)
    for d in range(1, group):
        across(lax.rem(mine + d, group), mine).start()
    own.start()
    for e in range(1, tp):
        within(x_ref, mine, lax.rem(mt + e, tp), mt).start()
    for d in range(1, group):
        b = lax.rem(mine - d + group, group)
        across(b, b).wait_recv()
        for e in range(1, tp):
            within(slot(b, mt), b, lax.rem(mt + e, tp), mt).start()
    own.wait()
    for d in range(1, group):
        across(lax.rem(mine + d, group), mine).wait_send()
    for d in range(group):
        b = lax.rem(mine - d + group, group)
        for e in range(1, tp):
            other = lax.rem(mt + e, tp)
            src = x_ref if d == 0 else slot(b, mt)
            within(src, b, other, mt).wait_send()
            within(src, b, other, other).wait_recv()


def gather_tokens(x, group, tp):
    rows, cols = x.shape
    dma = pltpu.SemaphoreType.DMA
    return pl.pallas_call(
        functools.partial(gather_kernel, group, tp),
        out_shape=jax.ShapeDtypeStruct((group * rows, tp * cols), x.dtype),
        in_specs=[VMEM],
        out_specs=VMEM,
        scratch_shapes=[dma, dma((group,)), dma((group,)), dma((group, tp)), dma((group, tp))],
        compiler_params=pltpu.CompilerParams(collective_id=1, has_side_effects=True, vmem_limit_bytes=40 << 20),
        name="gather_tokens",
    )(x)


def scatter_kernel(group, tp, part_ref, out_ref, arrived, summed, s1, r1, s2, r2):
    me, mt, base = greet_all(group, tp)
    mine = lax.rem(me, group)
    rows, cols = out_ref.shape[1:]

    def piece(b, t):
        return part_ref.at[
            pl.ds(pl.multiple_of(b * rows, rows), rows), pl.ds(pl.multiple_of(t * cols, cols), cols)
        ]

    def within(b, other, owner_t):
        return send_to(
            piece(b, other), arrived.at[b, owner_t], s1.at[b, other], r1.at[b, owner_t], {"sp": me, "tp": other}
        )

    def across(peer_b, owner_b):
        return send_to(
            summed.at[peer_b], out_ref.at[owner_b], s2.at[peer_b], r2.at[owner_b], {"sp": base + peer_b, "tp": mt}
        )

    for d in range(1, group + 1):
        b = lax.rem(mine + d, group)
        for e in range(1, tp):
            within(b, lax.rem(mt + e, tp), mt).start()
    for d in range(1, group + 1):
        b = lax.rem(mine + d, group)
        total = piece(b, mt)[...].astype(jnp.float32)
        for e in range(1, tp):
            other = lax.rem(mt + e, tp)
            within(b, other, other).wait_recv()
            total = total + arrived[b, other].astype(jnp.float32)
        if d < group:
            summed[b] = total.astype(jnp.bfloat16)
            across(b, mine).start()
        else:
            out_ref[mine] = total.astype(jnp.bfloat16)
    for d in range(1, group):
        b = lax.rem(mine + d, group)
        across(b, mine).wait_send()
        across(b, b).wait_recv()
    for b in range(group):
        for e in range(1, tp):
            within(b, lax.rem(mt + e, tp), mt).wait_send()


def scatter_sums(partials, group, tp):
    rows, cols = partials.shape[0] // group, partials.shape[1] // tp
    dma = pltpu.SemaphoreType.DMA
    return pl.pallas_call(
        functools.partial(scatter_kernel, group, tp),
        out_shape=jax.ShapeDtypeStruct((group, rows, cols), partials.dtype),
        in_specs=[VMEM],
        out_specs=VMEM,
        scratch_shapes=[
            pltpu.VMEM((group, tp, rows, cols), jnp.bfloat16),
            pltpu.VMEM((group, rows, cols), jnp.bfloat16),
            dma((group, tp)), dma((group, tp)), dma((group,)), dma((group,)),
        ],
        compiler_params=pltpu.CompilerParams(collective_id=2, has_side_effects=True, vmem_limit_bytes=40 << 20),
        name="scatter_sums",
    )(partials)


def local(
    n, tp, group,
    resid, queries, keys_values, cum_gate, out_weight, norm_gain,
    gate_weight, up_weight, conv_kernel, down_weight,
):
    tok_rows = resid.shape[0]
    wrows, hidden_cols = gate_weight.shape
    piece = hidden_cols // group
    wgu = jnp.concatenate(
        [gate_weight.reshape(wrows, group, piece), up_weight.reshape(wrows, group, piece)], axis=2
    ).transpose(1, 0, 2)
    wd = down_weight.reshape(group, piece, down_weight.shape[1])
    attn, wgu_all, wd_all = attend(queries, keys_values, cum_gate, wgu, wd, n, group)
    branch = jnp.dot(
        lax.all_gather(attn, "tp", axis=1, tiled=True),
        out_weight,
        preferred_element_type=jnp.float32,
    )
    middle = (resid.astype(jnp.float32) + branch).astype(jnp.bfloat16)
    middle_full = gather_tokens(middle, group, tp).astype(jnp.float32)
    inverse = lax.rsqrt(jnp.mean(middle_full * middle_full, axis=1, keepdims=True) + norm_eps)
    normed = (middle_full * inverse * norm_gain).astype(jnp.bfloat16)
    joined = jnp.dot(normed, wgu_all, preferred_element_type=jnp.float32).astype(jnp.bfloat16)
    taps = conv_kernel.shape[0]
    reach_back = taps - 1
    all_rows = joined.shape[0]
    pairs = [(i, i + group) for i in range(n) if i + group < n]
    before = lax.ppermute(joined[all_rows - reach_back :], "sp", pairs)
    padded = jnp.concatenate([before, joined], axis=0).astype(jnp.float32)
    at = lax.rem(lax.axis_index("sp"), group) * piece
    kernel = lax.dynamic_slice_in_dim(conv_kernel, at, piece, 2).reshape(taps, 2 * piece)
    mixed = jnp.zeros((all_rows, 2 * piece), jnp.float32)
    for offset in range(taps):
        mixed = mixed + kernel[offset][None, :] * padded[offset : offset + all_rows]
    hidden = (jax.nn.silu(mixed[:, :piece]) * mixed[:, piece:]).astype(jnp.bfloat16)
    partials = jnp.dot(hidden, wd_all, preferred_element_type=jnp.float32).astype(jnp.bfloat16)
    shares = scatter_sums(partials, group, tp).astype(jnp.float32)
    return (middle.astype(jnp.float32) + jnp.sum(shares, axis=0)).astype(jnp.bfloat16)


def solution(mesh):
    n, tp = mesh.shape["sp"], mesh.shape["tp"]
    group = next(g for g in (4, 2, 1) if n % g == 0)
    return jax.shard_map(
        functools.partial(local, n, tp, group),
        mesh=mesh,
        in_specs=(
            P("sp", "tp"),
            P("sp", "tp"),
            P("tp", "sp", None),
            P("tp", "sp"),
            P(None, "tp"),
            P(),
            P("sp", "tp"),
            P("sp", "tp"),
            P(None, None, "tp"),
            P("tp", "sp"),
        ),
        out_specs=P("sp", "tp"),
        check_vma=False,
    )
```

```python
import functools

import jax
import jax.numpy as jnp
from jax import lax
from jax.experimental import pallas as pl
from jax.experimental.pallas import tpu as pltpu
from jax.sharding import PartitionSpec as P

norm_eps = 1e-06
log2e = 1.4426950408889634
MESH = pl.DeviceIdType.MESH
VMEM = pl.BlockSpec(memory_space=pltpu.VMEM)
ANY = pl.BlockSpec(memory_space=pl.ANY)


def send_to(src, dst, send_sem, recv_sem, where):
    return pltpu.make_async_remote_copy(
        src_ref=src,
        dst_ref=dst,
        send_sem=send_sem,
        recv_sem=recv_sem,
        device_id=where,
        device_id_type=MESH,
    )


def attend_kernel(
    n, group, wide, q_ref, kv_ref, gate_ref, wgu_ref, wd_ref,
    out_ref, wgu_out, wd_out,
    kv_all, gate_all, max_s, acc_s,
    kv_send, kv_recv, gate_send, gate_recv, gu_send, gu_recv, dn_send, dn_recv, own_sem,
):
    me = lax.axis_index("sp")
    plane = n // group
    mine, place = me // plane, lax.rem(me, plane)
    pairs, rows, width = kv_ref.shape
    per_pair = gate_ref.shape[0] // pairs
    dcols = wd_ref.shape[2]

    barrier = pltpu.get_barrier_semaphore()

    def greet(peer):
        pl.semaphore_signal(barrier, inc=1, device_id={"sp": peer}, device_id_type=MESH)

    def greet_line(d, c):
        greet(lax.rem(mine + d, group) * plane + place)
        return c

    def greet_plane(e, c):
        greet(mine * plane + lax.rem(place + e, plane))
        return c

    lax.fori_loop(1, group, greet_line, 0)
    lax.fori_loop(1, plane, greet_plane, 0)
    pl.semaphore_wait(barrier, group + plane - 2)

    def kv_copy(src, owner, peer, at):
        return send_to(src, kv_all.at[owner], kv_send.at[at], kv_recv.at[owner], {"sp": peer})

    def gate_copy(src, owner, peer, at):
        return send_to(src, gate_all.at[owner], gate_send.at[at], gate_recv.at[owner], {"sp": peer})

    def wd_slot(owner):
        if wide:
            return wd_out.at[:, pl.ds(pl.multiple_of(owner * dcols, dcols), dcols)]
        return wd_out.at[owner]

    def gu_copy(src, owner, peer, at):
        return send_to(src, wgu_out.at[owner], gu_send.at[at], gu_recv.at[owner], {"sp": peer})

    def dn_copy(src, owner, peer, at):
        return send_to(src, wd_slot(owner), dn_send.at[at], dn_recv.at[owner], {"sp": peer})

    def line_kv(d, c):
        peer = (mine + d) * plane + place
        gate_copy(gate_ref, me, peer, peer).start()
        kv_copy(kv_ref, me, peer, peer).start()
        return c

    def own_plane_kv(e, c):
        peer = me + e
        gate_copy(gate_ref, me, peer, peer).start()
        kv_copy(kv_ref, me, peer, peer).start()
        return c

    lax.fori_loop(1, group - mine, line_kv, 0)
    lax.fori_loop(1, plane - place, own_plane_kv, 0)

    def line_weights(d, c):
        other = lax.rem(mine + d, group)
        peer = other * plane + place
        gu_copy(wgu_ref.at[other], me, peer, peer).start()
        dn_copy(wd_ref.at[other], me, peer, peer).start()
        return c

    lax.fori_loop(1, group, line_weights, 0)
    own_gu = pltpu.make_async_copy(wgu_ref.at[mine], wgu_out.at[me], own_sem.at[0])
    own_dn = pltpu.make_async_copy(wd_ref.at[mine], wd_slot(me), own_sem.at[1])
    own_gu.start()
    own_dn.start()

    def forward_kv(d, c):
        owner = (mine - d) * plane + place
        gate_copy(gate_ref, owner, me, me).wait_recv()
        kv_copy(kv_ref, owner, me, me).wait_recv()

        def out(e, c):
            to = lax.rem(place + e, plane)
            peer, at = mine * plane + to, (mine - d) * plane + to
            gate_copy(gate_all.at[owner], owner, peer, at).start()
            kv_copy(kv_all.at[owner], owner, peer, at).start()
            return c

        lax.fori_loop(1, plane, out, 0)
        return c

    lax.fori_loop(1, mine + 1, forward_kv, 0)

    def own_weights(e, c):
        peer = mine * plane + lax.rem(place + e, plane)
        gu_copy(wgu_ref.at[mine], me, peer, peer).start()
        dn_copy(wd_ref.at[mine], me, peer, peer).start()
        return c

    lax.fori_loop(1, plane, own_weights, 0)

    lanes = lax.broadcasted_iota(jnp.int32, (rows, width), 1)

    def fold(pair, block, gates, first):
        ones_values = jnp.where(lanes < width // 2, jnp.bfloat16(1.0), block)
        for inner in range(per_pair):
            h = pair * per_pair + inner
            scores = lax.dot_general(
                q_ref[h], block, (((1,), (1,)), ((), ())), preferred_element_type=jnp.float32
            )
            scores = scores * log2e - gates[h : h + 1, :] * log2e
            if first:
                r = lax.broadcasted_iota(jnp.int32, scores.shape, 0)
                c = lax.broadcasted_iota(jnp.int32, scores.shape, 1)
                scores = jnp.where(r >= c, scores, -1e30)
            top = jnp.max(scores, axis=1, keepdims=True)
            if first:
                weights = jnp.exp2(scores - top).astype(jnp.bfloat16)
                acc_s[h] = jnp.dot(weights, ones_values, preferred_element_type=jnp.float32)
                max_s[h] = jnp.broadcast_to(top, (scores.shape[0], width))
            else:
                old = max_s[h]
                top = jnp.maximum(old, top)
                weights = jnp.exp2(scores - top[:, :1]).astype(jnp.bfloat16)
                acc_s[h] = acc_s[h] * jnp.exp2(old - top) + jnp.dot(
                    weights, ones_values, preferred_element_type=jnp.float32
                )
                max_s[h] = top

    own_gates = gate_ref[...]
    for pair in range(pairs):
        fold(pair, kv_ref[pair], own_gates, True)

    def fold_owner(owner):
        gates = gate_all[owner]
        for pair in range(pairs):
            fold(pair, kv_all[owner, pair], gates, False)

    def stage(j, c):
        def from_plane(e, c):
            owner = (mine - j) * plane + lax.rem(place - e + plane, plane)
            gate_copy(gate_ref, owner, me, me).wait_recv()
            kv_copy(kv_ref, owner, me, me).wait_recv()
            fold_owner(owner)
            return c

        @pl.when(j > 0)
        def _():
            other = lax.rem(mine + j, group)
            owner = other * plane + place
            gu_copy(wgu_ref.at[mine], owner, me, me).wait_recv()
            dn_copy(wd_ref.at[mine], owner, me, me).wait_recv()

            def out(e, c):
                to = lax.rem(place + e, plane)
                peer, at = mine * plane + to, other * plane + to
                gu_copy(wgu_out.at[owner], owner, peer, at).start()
                dn_copy(wd_slot(owner), owner, peer, at).start()
                return c

            lax.fori_loop(1, plane, out, 0)

            @pl.when(j <= mine)
            def _():
                fold_owner((mine - j) * plane + place)

        count = jnp.where(j == 0, place + 1, jnp.where(j <= mine, plane, 1))
        lax.fori_loop(1, count, from_plane, 0)
        return c

    lax.fori_loop(0, group, stage, 0)
    for h in range(pairs * per_pair):
        acc = acc_s[h]
        out_ref[h] = (acc[:, width // 2 :] / acc[:, : width // 2]).astype(jnp.bfloat16)

    def end_kv(at):
        gate_copy(gate_ref, me, me, at).wait_send()
        kv_copy(kv_ref, me, me, at).wait_send()

    def end_line_kv(d, c):
        end_kv((mine + d) * plane + place)
        return c

    def end_plane_kv(e, c):
        end_kv(me + e)
        return c

    def end_forward_kv(d, c):
        def out(e, c):
            end_kv((mine - d) * plane + lax.rem(place + e, plane))
            return c

        lax.fori_loop(1, plane, out, 0)
        return c

    lax.fori_loop(1, group - mine, end_line_kv, 0)
    lax.fori_loop(1, plane - place, end_plane_kv, 0)
    lax.fori_loop(1, mine + 1, end_forward_kv, 0)

    def end_weights(at):
        gu_copy(wgu_ref.at[mine], me, me, at).wait_send()
        dn_copy(wd_ref.at[mine], me, me, at).wait_send()

    def end_line(d, c):
        end_weights(lax.rem(mine + d, group) * plane + place)
        return c

    lax.fori_loop(1, group, end_line, 0)

    def end_plane(k, c):
        def out(e, c):
            at = k * plane + lax.rem(place + e, plane)
            end_weights(at)
            gu_copy(wgu_ref.at[mine], at, me, me).wait_recv()
            dn_copy(wd_ref.at[mine], at, me, me).wait_recv()
            return c

        lax.fori_loop(1, plane, out, 0)
        return c

    lax.fori_loop(0, group, end_plane, 0)
    own_gu.wait()
    own_dn.wait()


def attend(queries, keys_values, cum_gate, wgu, wd, n, group):
    tok_rows = queries.shape[0]
    pairs, rows, width = keys_values.shape
    heads = cum_gate.shape[0]
    head_dim = width // 2
    q = (queries * (head_dim**-0.5)).astype(jnp.bfloat16).reshape(tok_rows, heads, head_dim)
    q = jnp.pad(q.transpose(1, 0, 2), ((0, 0), (0, 0), (0, head_dim)))
    _, hid, dcols = wd.shape
    wide = dcols % 128 == 0
    dma = pltpu.SemaphoreType.DMA
    out, wgu_all, wd_all = pl.pallas_call(
        functools.partial(attend_kernel, n, group, wide),
        out_shape=(
            jax.ShapeDtypeStruct((heads, tok_rows, head_dim), jnp.bfloat16),
            jax.ShapeDtypeStruct((n,) + wgu.shape[1:], jnp.bfloat16),
            jax.ShapeDtypeStruct((hid, n * dcols) if wide else (n, hid, dcols), jnp.bfloat16),
        ),
        in_specs=[VMEM] * 5,
        out_specs=(VMEM, ANY, ANY),
        scratch_shapes=[
            pltpu.VMEM((n, pairs, rows, width), jnp.bfloat16),
            pltpu.VMEM((n, heads, rows), jnp.float32),
            pltpu.VMEM((heads, tok_rows, width), jnp.float32),
            pltpu.VMEM((heads, tok_rows, width), jnp.float32),
        ]
        + [dma((n,))] * 8
        + [dma((2,))],
        compiler_params=pltpu.CompilerParams(collective_id=0, has_side_effects=True, vmem_limit_bytes=40 << 20),
        cost_estimate=pl.CostEstimate(flops=10**10, bytes_accessed=10**7, transcendentals=10**7),
        name="attend",
    )(q, keys_values, cum_gate, wgu, wd)
    if not wide:
        wd_all = wd_all.transpose(1, 0, 2).reshape(hid, n * dcols)
    attn = out.transpose(1, 0, 2).reshape(tok_rows, heads * head_dim)
    return attn, wgu_all.reshape(-1, wgu.shape[2]), wd_all


def greet_all(plane, group, tp):
    me, mt = lax.axis_index("sp"), lax.axis_index("tp")
    mine, place = me // plane, lax.rem(me, plane)
    barrier = pltpu.get_barrier_semaphore()
    for d in range(1, group):
        peer = lax.rem(mine + d, group) * plane + place
        pl.semaphore_signal(barrier, inc=1, device_id={"sp": peer, "tp": mt}, device_id_type=MESH)
    for e in range(1, tp):
        other = lax.rem(mt + e, tp)
        pl.semaphore_signal(barrier, inc=1, device_id={"sp": me, "tp": other}, device_id_type=MESH)
    pl.semaphore_wait(barrier, group + tp - 2)
    return me, mt, mine, place


def gather_kernel(plane, group, tp, x_ref, out_ref, own_sem, s1, r1, s2, r2):
    rows, cols = x_ref.shape
    me, mt, mine, place = greet_all(plane, group, tp)

    def slot(b, t):
        return out_ref.at[
            pl.ds(pl.multiple_of(b * rows, rows), rows), pl.ds(pl.multiple_of(t * cols, cols), cols)
        ]

    def across(peer_b, owner_b):
        return send_to(
            x_ref, slot(owner_b, mt), s1.at[peer_b], r1.at[owner_b], {"sp": peer_b * plane + place, "tp": mt}
        )

    def within(src, b, other, owner_t):
        return send_to(src, slot(b, owner_t), s2.at[b, other], r2.at[b, owner_t], {"sp": me, "tp": other})

    own = pltpu.make_async_copy(x_ref, slot(mine, mt), own_sem)
    for d in range(1, group):
        across(lax.rem(mine + d, group), mine).start()
    own.start()
    for e in range(1, tp):
        within(x_ref, mine, lax.rem(mt + e, tp), mt).start()
    for d in range(1, group):
        b = lax.rem(mine - d + group, group)
        across(b, b).wait_recv()
        for e in range(1, tp):
            within(slot(b, mt), b, lax.rem(mt + e, tp), mt).start()
    own.wait()
    for d in range(1, group):
        across(lax.rem(mine + d, group), mine).wait_send()
    for d in range(group):
        b = lax.rem(mine - d + group, group)
        for e in range(1, tp):
            other = lax.rem(mt + e, tp)
            src = x_ref if d == 0 else slot(b, mt)
            within(src, b, other, mt).wait_send()
            within(src, b, other, other).wait_recv()


def gather_tokens(x, plane, group, tp):
    rows, cols = x.shape
    dma = pltpu.SemaphoreType.DMA
    return pl.pallas_call(
        functools.partial(gather_kernel, plane, group, tp),
        out_shape=jax.ShapeDtypeStruct((group * rows, tp * cols), x.dtype),
        in_specs=[VMEM],
        out_specs=VMEM,
        scratch_shapes=[dma, dma((group,)), dma((group,)), dma((group, tp)), dma((group, tp))],
        compiler_params=pltpu.CompilerParams(collective_id=1, has_side_effects=True, vmem_limit_bytes=40 << 20),
        name="gather_tokens",
    )(x)


def scatter_kernel(plane, group, tp, part_ref, out_ref, arrived, summed, s1, r1, s2, r2):
    me, mt, mine, place = greet_all(plane, group, tp)
    rows, cols = out_ref.shape[1:]

    def piece(b, t):
        return part_ref.at[
            pl.ds(pl.multiple_of(b * rows, rows), rows), pl.ds(pl.multiple_of(t * cols, cols), cols)
        ]

    def within(b, other, owner_t):
        return send_to(
            piece(b, other), arrived.at[b, owner_t], s1.at[b, other], r1.at[b, owner_t], {"sp": me, "tp": other}
        )

    def across(peer_b, owner_b):
        return send_to(
            summed.at[peer_b], out_ref.at[owner_b], s2.at[peer_b], r2.at[owner_b], {"sp": peer_b * plane + place, "tp": mt}
        )

    for d in range(1, group + 1):
        b = lax.rem(mine + d, group)
        for e in range(1, tp):
            within(b, lax.rem(mt + e, tp), mt).start()
    for d in range(1, group + 1):
        b = lax.rem(mine + d, group)
        total = piece(b, mt)[...].astype(jnp.float32)
        for e in range(1, tp):
            other = lax.rem(mt + e, tp)
            within(b, other, other).wait_recv()
            total = total + arrived[b, other].astype(jnp.float32)
        if d < group:
            summed[b] = total.astype(jnp.bfloat16)
            across(b, mine).start()
        else:
            out_ref[mine] = total.astype(jnp.bfloat16)
    for d in range(1, group):
        b = lax.rem(mine + d, group)
        across(b, mine).wait_send()
        across(b, b).wait_recv()
    for b in range(group):
        for e in range(1, tp):
            within(b, lax.rem(mt + e, tp), mt).wait_send()


def scatter_sums(partials, plane, group, tp):
    rows, cols = partials.shape[0] // group, partials.shape[1] // tp
    dma = pltpu.SemaphoreType.DMA
    return pl.pallas_call(
        functools.partial(scatter_kernel, plane, group, tp),
        out_shape=jax.ShapeDtypeStruct((group, rows, cols), partials.dtype),
        in_specs=[VMEM],
        out_specs=VMEM,
        scratch_shapes=[
            pltpu.VMEM((group, tp, rows, cols), jnp.bfloat16),
            pltpu.VMEM((group, rows, cols), jnp.bfloat16),
            dma((group, tp)), dma((group, tp)), dma((group,)), dma((group,)),
        ],
        compiler_params=pltpu.CompilerParams(collective_id=2, has_side_effects=True, vmem_limit_bytes=40 << 20),
        name="scatter_sums",
    )(partials)


def local(
    n, tp, group,
    resid, queries, keys_values, cum_gate, out_weight, norm_gain,
    gate_weight, up_weight, conv_kernel, down_weight,
):
    tok_rows = resid.shape[0]
    plane = n // group
    place = lax.rem(lax.axis_index("sp"), plane)
    wrows, hidden_cols = gate_weight.shape
    piece = hidden_cols // group
    wgu = jnp.concatenate(
        [gate_weight.reshape(wrows, group, piece), up_weight.reshape(wrows, group, piece)], axis=2
    ).transpose(1, 0, 2)
    wd = down_weight.reshape(group, piece, down_weight.shape[1])
    attn, wgu_all, wd_all = attend(queries, keys_values, cum_gate, wgu, wd, n, group)
    branch = jnp.dot(
        lax.all_gather(attn, "tp", axis=1, tiled=True),
        out_weight,
        preferred_element_type=jnp.float32,
    )
    middle = (resid.astype(jnp.float32) + branch).astype(jnp.bfloat16)
    middle_full = gather_tokens(middle, plane, group, tp).astype(jnp.float32)
    inverse = lax.rsqrt(jnp.mean(middle_full * middle_full, axis=1, keepdims=True) + norm_eps)
    normed = (middle_full * inverse * norm_gain).astype(jnp.bfloat16)
    joined = jnp.dot(normed, wgu_all, preferred_element_type=jnp.float32).astype(jnp.bfloat16)
    taps = conv_kernel.shape[0]
    reach_back = taps - 1
    blocks = joined.reshape(group, tok_rows, 2 * piece)
    pairs = [(i, i - i % plane + (i + 1) % plane) for i in range(n)]
    before = lax.ppermute(blocks[:, tok_rows - reach_back :], "sp", pairs)
    shifted = jnp.concatenate([jnp.zeros_like(before[:1]), before[:-1]], axis=0)
    before = jnp.where(place == 0, shifted, before)
    padded = jnp.concatenate([before, blocks], axis=1).astype(jnp.float32)
    at = (lax.axis_index("sp") // plane) * piece
    kernel = lax.dynamic_slice_in_dim(conv_kernel, at, piece, 2).reshape(taps, 2 * piece)
    mixed = jnp.zeros((group, tok_rows, 2 * piece), jnp.float32)
    for offset in range(taps):
        mixed = mixed + kernel[offset][None, None, :] * padded[:, offset : offset + tok_rows]
    mixed = mixed.reshape(group * tok_rows, 2 * piece)
    hidden = (jax.nn.silu(mixed[:, :piece]) * mixed[:, piece:]).astype(jnp.bfloat16)
    partials = jnp.dot(hidden, wd_all, preferred_element_type=jnp.float32).astype(jnp.bfloat16)
    shares = scatter_sums(partials, plane, group, tp).astype(jnp.float32)
    return (middle.astype(jnp.float32) + jnp.sum(shares, axis=0)).astype(jnp.bfloat16)


def solution(mesh):
    n, tp = mesh.shape["sp"], mesh.shape["tp"]
    group = next(g for g in (4, 2, 1) if n % g == 0)
    return jax.shard_map(
        functools.partial(local, n, tp, group),
        mesh=mesh,
        in_specs=(
            P("sp", "tp"),
            P("sp", "tp"),
            P("tp", "sp", None),
            P("tp", "sp"),
            P(None, "tp"),
            P(),
            P("sp", "tp"),
            P("sp", "tp"),
            P(None, None, "tp"),
            P("tp", "sp"),
        ),
        out_specs=P("sp", "tp"),
        check_vma=False,
    )
```
